32 devices in a mesh: sp: 8 (over z, core), tp: 4 (over y, x).
Axes of the slice: x: 2, y: 2, z: 4, core: 2. Of those that a mesh axis runs over, the one named last changes fastest.
Arguments:
- u_val: bfloat16 [2048, 2048], P('sp', 'tp'), may hold values from -6 to 6
- u_gate: bfloat16 [2048, 2048], P('sp', 'tp'), may hold values from -9 to 9
- conv_weight: float32 [31, 2048], P(None, 'tp')
- conv_bias: float32 [2048], P('tp'), may hold values from -3 to 3
- ln_gain: float32 [2048], P('tp'), may hold values from 0.1 to 1.9
- ln_bias: float32 [2048], P('tp'), may hold values from -3 to 3
- proj_weight: bfloat16 [2048, 4096], P(None, 'tp'), may hold values from -0.125 to 0.125
- resid: bfloat16 [2048, 4096], P('sp', 'tp')
- norm_gain: float32 [4096], P('tp'), may hold values from 0.1 to 1.9
- route_ids: int32 [2048, 2], P('sp'), may hold values from 0 to 7, all different within a row; in each aligned block of 256 rows (0 to 255, 256 to 511, ...) at most 128 rows name the same one
- route_wts: float32 [2048, 2], P('sp'), may hold values from 0.3 to 1.5
- expert_gate: bfloat16 [8, 4096, 1024], P('sp', None, 'tp'), may hold values from -0.09375 to 0.09375
- expert_up: bfloat16 [8, 4096, 1024], P('sp', None, 'tp'), may hold values from -0.09375 to 0.09375
- expert_down: bfloat16 [8, 1024, 4096], P('sp', None, 'tp'), may hold values from -0.1875 to 0.1875
- shared_gate: bfloat16 [4096, 1024], P(None, 'tp'), may hold values from -0.09375 to 0.09375
- shared_up: bfloat16 [4096, 1024], P(None, 'tp'), may hold values from -0.09375 to 0.09375
- shared_down: bfloat16 [1024, 4096], P(None, 'tp'), may hold values from -0.1875 to 0.1875
Outputs:
- mixed: bfloat16 [2048, 4096], P('sp', 'tp')
The draws below stay inside these ranges and needn't reach their ends.
Inputs may be any that keep to these rules, and one draw needn't show every extreme that they name: `route_ids`: each row names 2 different experts. In each aligned block of 256 rows (the rows of one index of sp) no expert is named by more than 128 rows, a bound that some expert reaches in some blocks.
All inputs are finite; a program needn't handle non-finite values.
Results may differ from the reference program's by a relative error of at most 0.012.
Values may be sent and summed in bfloat16 or wider, within the bound.
No kernel may reach another device: no remote copies, remote signals or barrier semaphores. Data moves between devices by JAX's collectives and lax.ppermute only.
A program may use at most 64 MiB of HBM per device.

```python
import math
import jax
import jax.numpy as jnp
import numpy as np
from jax import lax

D = 4096
CONV = 2048
EXPERT_HIDDEN = 1024
SHARED_HIDDEN = 1024
KERNEL = 31
TOP = 2
TOK_DEV = 256
TOKENS = 2048
EXPERTS = 8
CAP = 128
N_SP = 8


def draw_conv_weight(key, part):
    ramp = 4.0 ** (jnp.arange(CONV, dtype=jnp.float32) / (CONV - 1))
    base = jax.random.normal(key, (KERNEL, CONV), jnp.float32)
    return base * ramp[None, :] * KERNEL ** (-0.5)


def draw_resid(key, part):
    ramp = 3.0 ** (jnp.arange(D, dtype=jnp.float32) / (D - 1))
    base = jax.random.normal(key, (TOKENS, D), jnp.float32)
    return (base * ramp[None, :]).astype(jnp.bfloat16)


def levels(stream_key, shape, split, low, largest):
    def one(dim, blocks):
        steps = jax.random.uniform(jax.random.fold_in(jax.random.fold_in(stream_key, 6), dim), (blocks,), jnp.float32, low / len(split), largest / len(split))
        return jnp.repeat(jnp.exp(steps), shape[dim] // blocks).reshape((-1,) + (1,) * (len(shape) - dim - 1))

    gain = one(*split[0])
    for cut in split[1:]:
        gain = gain * one(*cut)
    return gain


def deal_out(own_key, own, number, rows, count, top, bound, lean):
    order = jax.random.permutation(own_key, count)
    crowded, common = shares(count, rows * top, bound, lean, True), shares(count, rows * top, bound, lean, False)
    places = jnp.arange(count)

    def named(tallies, offset_by):
        used = int((tallies > 0).sum())
        fixed = max(1, used // 4)
        moved = fixed + (places - fixed + offset_by * (used - fixed)) % max(1, count - fixed)
        return jnp.zeros((count,), jnp.int32).at[order[jnp.where(places < fixed, places, moved)]].set(jnp.asarray(tallies, jnp.int32))

    tallies = jnp.where(number % 4 == 0, named(crowded, number // 4), named(common, number - number // 4 - 1))
    mixed = jax.random.permutation(jax.random.fold_in(own, 3), count)
    source_of, taker = mixed[0:count // 2 * 2:2], mixed[1:count // 2 * 2:2]
    room = jnp.minimum(tallies[source_of] - 1, bound - tallies[taker]) // 2
    room = jnp.where((source_of == order[0]) | (taker == order[0]) | (tallies[taker] == 0), 0, jnp.maximum(room, 0))
    moved = jax.random.randint(jax.random.fold_in(own, 4), (count // 2,), 0, 1 << 20) % (room + 1)
    tallies = tallies.at[source_of].add(-moved).at[taker].add(moved)
    members = jnp.searchsorted(jnp.cumsum(tallies), jnp.arange(rows * top), side="right").astype(jnp.int32)
    listing = members.reshape(top, rows).T
    listing = listing[jax.random.permutation(jax.random.fold_in(own, 1), rows)]
    offset_by = jax.random.randint(jax.random.fold_in(own, 2), (rows, 1), 0, top)
    return jnp.take_along_axis(listing, (jnp.arange(top)[None, :] + offset_by) % top, axis=1)


def shares(amount, total, reach, lean, full):
    portions = [(1 << 20) // math.isqrt(standing ** lean) + 1 for standing in range(1, amount + 1)]
    largest = reach if full else min(reach, max(-(-total // amount), total * portions[0] // sum(portions)))
    least = 1 if total - largest >= amount - 1 else 0
    holding, rest = [largest] + [least] * (amount - 1), total - largest - least * (amount - 1)
    while rest > 0:
        free = [i for i in range(1, amount) if holding[i] < largest] or [i for i in range(1, amount) if holding[i] < reach]
        whole, left = sum([portions[i] for i in free]), rest
        for i in free:
            more = min(reach - holding[i], max(1, left * portions[i] // whole), rest)
            holding[i] = holding[i] + more
            rest = rest - more
    return np.array(holding)


def normal_values(stream_key, shape, scale, reach, split=(), kind=jnp.bfloat16):
    drawn = jax.random.normal(stream_key, shape, jnp.float32) * scale
    if len(split) > 0:
        drawn = levels(stream_key, shape, split, -0.22, 0.18) * drawn
    return jnp.clip(drawn, min=-reach, max=reach).astype(kind)


def setup_inputs(seed: int = 0) -> dict:
    arg_keys = jax.random.split(jax.random.key(seed), 18)
    u_val = normal_values(arg_keys[0], (TOKENS, CONV), 1.0, 6.0, ((0, 8), (1, 4)))
    u_gate = normal_values(arg_keys[1], (TOKENS, CONV), 1.5, 9.0, ((0, 8), (1, 4)))
    conv_weight = draw_conv_weight(jax.random.fold_in(arg_keys[17], 71), 0)
    conv_bias = normal_values(arg_keys[3], (CONV,), 0.5, 3.0, ((0, 4),), jnp.float32)
    ln_gain = jnp.clip(1.0 + 0.18 * jax.random.normal(arg_keys[4], (CONV,), jnp.float32), 0.1, 1.9)
    ln_bias = normal_values(arg_keys[5], (CONV,), 0.5, 3.0, ((0, 4),), jnp.float32)
    proj_weight = normal_values(arg_keys[6], (CONV, D), CONV ** -0.5, 0.125, ((1, 4),))
    resid = draw_resid(jax.random.fold_in(arg_keys[17], 71), 0)
    norm_gain = jnp.clip(1.0 + 0.18 * jax.random.normal(arg_keys[8], (D,), jnp.float32), 0.1, 1.9)
    route_ids_keys = jax.random.split(jax.random.fold_in(arg_keys[9], 1), TOKENS // TOK_DEV)
    route_ids_turns = jax.random.permutation(jax.random.fold_in(arg_keys[9], 3), TOKENS // TOK_DEV)
    route_ids = jax.vmap(lambda own, number: deal_out(jax.random.fold_in(arg_keys[9], 2), own, number, TOK_DEV, EXPERTS, TOP, CAP, 2))(route_ids_keys, route_ids_turns).reshape((TOKENS, TOP))
    route_wts = jnp.clip(0.3 + 1.2 * jax.random.uniform(arg_keys[10], (TOKENS, TOP), jnp.float32) ** levels(arg_keys[10], (TOKENS, TOP), ((0, 8),), -0.2, 0.2), 0.3, 1.5)
    expert_gate = normal_values(arg_keys[11], (EXPERTS, D, EXPERT_HIDDEN), D ** -0.5, 0.09375, ((0, 8), (2, 4)))
    expert_up = normal_values(arg_keys[12], (EXPERTS, D, EXPERT_HIDDEN), D ** -0.5, 0.09375, ((0, 8), (2, 4)))
    expert_down = normal_values(arg_keys[13], (EXPERTS, EXPERT_HIDDEN, D), EXPERT_HIDDEN ** -0.5, 0.1875, ((0, 8), (2, 4)))
    shared_gate = normal_values(arg_keys[14], (D, SHARED_HIDDEN), D ** -0.5, 0.09375, ((1, 4),))
    shared_up = normal_values(arg_keys[15], (D, SHARED_HIDDEN), D ** -0.5, 0.09375, ((1, 4),))
    shared_down = normal_values(arg_keys[16], (SHARED_HIDDEN, D), SHARED_HIDDEN ** -0.5, 0.1875, ((1, 4),))
    return {"u_val": u_val, "u_gate": u_gate, "conv_weight": conv_weight, "conv_bias": conv_bias, "ln_gain": ln_gain, "ln_bias": ln_bias, "proj_weight": proj_weight, "resid": resid, "norm_gain": norm_gain, "route_ids": route_ids, "route_wts": route_wts, "expert_gate": expert_gate, "expert_up": expert_up, "expert_down": expert_down, "shared_gate": shared_gate, "shared_up": shared_up, "shared_down": shared_down}


norm_eps = 1e-06

def slot_table(block_ids, block_wts):
    pair_ids = block_ids.reshape(-1)
    pair_wts = block_wts.reshape(-1)
    onehot = (pair_ids[:, None] == jnp.arange(EXPERTS, dtype=jnp.int32)[None, :]).astype(jnp.int32)
    before = jnp.cumsum(onehot, axis=0) - onehot
    position = lax.optimization_barrier(jnp.sum(before * onehot, axis=1))
    pair_slot = pair_ids * CAP + position
    matches = (jnp.arange(EXPERTS * CAP, dtype=jnp.int32)[:, None] == pair_slot[None, :]).astype(jnp.int32)
    pair_tok = (jnp.arange(TOK_DEV * TOP, dtype=jnp.int32) // TOP).astype(jnp.int32)
    filled = lax.optimization_barrier(jnp.sum(matches, axis=1))
    slot_tok = lax.optimization_barrier(jnp.sum(matches * pair_tok[None, :], axis=1)) + (1 - filled) * TOK_DEV
    slot_wts = lax.optimization_barrier(jnp.sum(matches.astype(jnp.float32) * pair_wts[None, :], axis=1))
    return (slot_tok.astype(jnp.int32), slot_wts)

def reference(u_val, u_gate, conv_weight, conv_bias, ln_gain, ln_bias, proj_weight, resid, norm_gain, route_ids, route_wts, expert_gate, expert_up, expert_down, shared_gate, shared_up, shared_down):
    gated = (u_val.astype(jnp.float32) * jax.nn.sigmoid(u_gate.astype(jnp.float32))).astype(jnp.bfloat16)
    gated = lax.optimization_barrier(gated).astype(jnp.float32)
    padded = jnp.concatenate([jnp.zeros((KERNEL - 1, CONV), jnp.float32), gated], axis=0)
    conv_sum = jnp.zeros((TOKENS, CONV), jnp.float32) + conv_bias[None, :]
    for tap_index in range(KERNEL):
        conv_sum = conv_sum + conv_weight[tap_index][None, :] * padded[tap_index:tap_index + TOKENS]
    channel_mean = lax.optimization_barrier(jnp.mean(conv_sum, axis=1, keepdims=True))
    centered = conv_sum - channel_mean
    channel_var = lax.optimization_barrier(jnp.mean(centered * centered, axis=1, keepdims=True))
    conv_out = jax.nn.silu(centered * lax.rsqrt(channel_var + norm_eps) * ln_gain + ln_bias).astype(jnp.bfloat16)
    projected = jnp.dot(conv_out, proj_weight, preferred_element_type=jnp.float32)
    residual_mid = (resid.astype(jnp.float32) + projected).astype(jnp.bfloat16)
    residual_wide = residual_mid.astype(jnp.float32)
    mean_square = lax.optimization_barrier(jnp.mean(residual_wide * residual_wide, axis=1, keepdims=True))
    normed_rows = (residual_wide * lax.rsqrt(mean_square + norm_eps) * norm_gain).astype(jnp.bfloat16)
    shared_hidden = (jax.nn.silu(jnp.dot(normed_rows, shared_gate, preferred_element_type=jnp.float32)) * jnp.dot(normed_rows, shared_up, preferred_element_type=jnp.float32)).astype(jnp.bfloat16)
    shared_out = jnp.dot(shared_hidden, shared_down, preferred_element_type=jnp.float32)
    slot_tok, slot_wts = jax.vmap(slot_table)(route_ids.reshape(N_SP, TOK_DEV, TOP), route_wts.reshape(N_SP, TOK_DEV, TOP))
    offsets = (jnp.arange(N_SP, dtype=jnp.int32) * TOK_DEV)[:, None]
    global_tok = jnp.where(slot_tok < TOK_DEV, slot_tok + offsets, TOKENS).astype(jnp.int32)
    global_tok = global_tok.reshape(N_SP, EXPERTS, CAP).transpose(1, 0, 2).reshape(EXPERTS, N_SP * CAP)
    slot_wts = slot_wts.reshape(N_SP, EXPERTS, CAP).transpose(1, 0, 2).reshape(EXPERTS, N_SP * CAP)
    rows_ext = jnp.concatenate([normed_rows, jnp.zeros((1, D), jnp.bfloat16)], axis=0)

    def expert_step(total, inputs):
        gate_w, up_w, down_w, tok_ids, tok_wts = inputs
        slot_rows = jnp.take(rows_ext, tok_ids, axis=0)
        hidden = (jax.nn.silu(jnp.dot(slot_rows, gate_w, preferred_element_type=jnp.float32)) * jnp.dot(slot_rows, up_w, preferred_element_type=jnp.float32)).astype(jnp.bfloat16)
        expert_out = jnp.dot(hidden, down_w, preferred_element_type=jnp.float32).astype(jnp.bfloat16)
        weighted = expert_out.astype(jnp.float32) * tok_wts[:, None]
        return (total + jax.ops.segment_sum(weighted, tok_ids, num_segments=TOKENS + 1), None)
    routed, _ = lax.scan(expert_step, jnp.zeros((TOKENS + 1, D), jnp.float32), (expert_gate, expert_up, expert_down, global_tok, slot_wts))
    return (residual_wide + shared_out + routed[:TOKENS]).astype(jnp.bfloat16)
```

```python
import jax
import jax.numpy as jnp
from jax import lax
from jax.experimental import pallas as pl
from jax.experimental.pallas import tpu as pltpu
from jax.sharding import PartitionSpec as P

norm_eps = 1e-06
PERMUTE_LIMIT = 8
F32 = jnp.float32
BF16 = jnp.bfloat16


def xor_permute(block, axis, k):
    n = lax.axis_size(axis)
    return lax.ppermute(block, axis, [(i, i ^ k) for i in range(n)])


def spread(block, axis):
    n = lax.axis_size(axis)
    if n <= PERMUTE_LIMIT:
        return [block] + [xor_permute(block, axis, k) for k in range(1, n)]
    everyone = lax.all_gather(block, axis)
    me = lax.axis_index(axis)
    return [lax.dynamic_index_in_dim(everyone, me ^ k, 0, keepdims=False) for k in range(n)]


def swap(blocks, axis, places):
    n = lax.axis_size(axis)
    return {k: blocks[k] if k == 0 else xor_permute(blocks[k], axis, k) for k in places}


def silu(v):
    return v / (1.0 + jnp.exp(-v))


def whole_spec(count):
    return [pl.BlockSpec(memory_space=pltpu.VMEM) for _ in range(count)]


def call(body, me, operands, out):
    return pl.pallas_call(
        body,
        in_specs=[pl.BlockSpec(memory_space=pltpu.SMEM)] + whole_spec(len(operands)),
        out_specs=pl.BlockSpec(memory_space=pltpu.VMEM),
        out_shape=out,
    )(me, *operands)


def project(me, parts, gains, biases, stats, proj_weight, resid):
    n = len(parts)

    def body(me_ref, *refs):
        part_refs, gain_ref, bias_ref, stat_ref, w_ref, resid_ref, out_ref = (
            refs[:n], refs[n], refs[n + 1], refs[n + 2], refs[n + 3], refs[n + 4], refs[n + 5]
        )
        width = part_refs[0].shape[1]
        rstd = stat_ref[:, n : n + 1]
        total = resid_ref[...].astype(F32)
        for k in range(n):
            v = (part_refs[k][...].astype(F32) + stat_ref[:, k : k + 1]) * rstd
            v = silu(v * gain_ref[k : k + 1, :] + bias_ref[k : k + 1, :]).astype(BF16)
            start = pl.multiple_of((me_ref[0] ^ k) * width, width)
            total = total + jnp.dot(v, w_ref[pl.ds(start, width), :], preferred_element_type=F32)
        out_ref[...] = total.astype(BF16)

    return call(
        body, me, [*parts, gains, biases, stats, proj_weight, resid],
        jax.ShapeDtypeStruct(resid.shape, BF16),
    )


def expert_in(me, parts, gains, gate, up):
    n = len(parts)

    def body(me_ref, *refs):
        part_refs, gain_ref, gate_ref, up_ref, out_ref = refs[:n], refs[n], refs[n + 1], refs[n + 2], refs[n + 3]
        width = part_refs[0].shape[1]
        squares = 0.0
        for k in range(n):
            v = part_refs[k][...].astype(F32)
            squares = squares + jnp.sum(v * v, axis=1, keepdims=True)
        scale = lax.rsqrt(squares / (n * width) + norm_eps)
        gate_sum = up_sum = 0.0
        for k in range(n):
            v = (part_refs[k][...].astype(F32) * scale * gain_ref[k : k + 1, :]).astype(BF16)
            start = pl.multiple_of((me_ref[0] ^ k) * width, width)
            gate_sum = gate_sum + jnp.dot(v, gate_ref[pl.ds(start, width), :], preferred_element_type=F32)
            up_sum = up_sum + jnp.dot(v, up_ref[pl.ds(start, width), :], preferred_element_type=F32)
        out_ref[...] = (silu(gate_sum) * up_sum).astype(BF16)

    return call(
        body, me, [*parts, gains, gate, up],
        jax.ShapeDtypeStruct((parts[0].shape[0], gate.shape[1]), BF16),
    )


def expert_out(me, parts, down):
    n = len(parts)

    def body(me_ref, *refs):
        part_refs, down_ref, out_ref = refs[:n], refs[n], refs[n + 1]
        width = part_refs[0].shape[1]
        total = 0.0
        for k in range(n):
            start = pl.multiple_of((me_ref[0] ^ k) * width, width)
            total = total + jnp.dot(part_refs[k][...], down_ref[pl.ds(start, width), :], preferred_element_type=F32)
        out_ref[...] = total.astype(BF16)

    return call(
        body, me, [*parts, down],
        jax.ShapeDtypeStruct((parts[0].shape[0], down.shape[1]), BF16),
    )


def combine(me, parts, down, residual, slots, weights, returned):
    n, m = len(parts), len(returned)

    def body(me_ref, *refs):
        part_refs, down_ref, residual_ref, slot_ref, weight_ref = (
            refs[:n], refs[n], refs[n + 1], refs[n + 2], refs[n + 3]
        )
        back_refs, out_ref = refs[n + 4 : n + 4 + m], refs[n + 4 + m]
        width = part_refs[0].shape[1]
        total = residual_ref[...].astype(F32)
        for k in range(n):
            start = pl.multiple_of((me_ref[0] ^ k) * width, width)
            total = total + jnp.dot(part_refs[k][...], down_ref[pl.ds(start, width), :], preferred_element_type=F32)
        count = back_refs[0].shape[0]
        for g in range(m):
            places = lax.broadcasted_iota(jnp.int32, (residual_ref.shape[0], count), 1) + g * count
            picked = 0.0
            for j in range(slot_ref.shape[1]):
                picked = picked + jnp.where(places == slot_ref[:, j : j + 1], weight_ref[:, j : j + 1], 0.0)
            high = picked.astype(BF16)
            low = (picked - high.astype(F32)).astype(BF16)
            total = total + jnp.dot(high, back_refs[g][...], preferred_element_type=F32)
            total = total + jnp.dot(low, back_refs[g][...], preferred_element_type=F32)
        out_ref[...] = total.astype(BF16)

    return call(
        body, me, [*parts, down, residual, slots, weights, *returned],
        jax.ShapeDtypeStruct(residual.shape, BF16),
    )


def shards(
    u_val,
    u_gate,
    conv_weight,
    conv_bias,
    ln_gain,
    ln_bias,
    proj_weight,
    resid,
    norm_gain,
    route_ids,
    route_wts,
    expert_gate,
    expert_up,
    expert_down,
    shared_gate,
    shared_up,
    shared_down,
):
    tok_rows, channels = u_val.shape
    sp_count = lax.axis_size("sp")
    tp_count = lax.axis_size("tp")
    sp_me = lax.axis_index("sp")
    me = lax.axis_index("tp").astype(jnp.int32).reshape(1)
    kernel_width = conv_weight.shape[0]
    topk_count = route_ids.shape[1]
    capacity = 2 * tok_rows * topk_count // sp_count

    gated = (u_val.astype(F32) * jax.nn.sigmoid(u_gate.astype(F32))).astype(BF16)
    ends = gated[tok_rows - (kernel_width - 1) :]
    rim_rows = lax.ppermute(ends, "sp", [(i, i + 1) for i in range(sp_count - 1)])
    vectors = spread(jnp.concatenate([ln_gain, ln_bias, norm_gain]), "tp")
    padded = lax.optimization_barrier(jnp.concatenate([rim_rows, gated], axis=0)).astype(F32)
    conv_sum = jnp.zeros((tok_rows, channels), F32) + conv_bias[None, :]
    for tap_index in range(kernel_width):
        conv_sum = conv_sum + conv_weight[tap_index][None, :] * padded[tap_index : tap_index + tok_rows]
    own_mean = jnp.mean(conv_sum, axis=1)
    centred = conv_sum - own_mean[:, None]
    own_squares = jnp.sum(centred * centred, axis=1)
    conv_parts = spread(centred.astype(BF16), "tp")
    stat_parts = spread(jnp.stack([own_mean, own_squares]), "tp")
    means = jnp.stack([s[0] for s in stat_parts])
    channel_mean = jnp.mean(means, axis=0)
    shifts = means - channel_mean
    spread_sum = sum(s[1] for s in stat_parts) + channels * jnp.sum(shifts * shifts, axis=0)
    rstd = lax.rsqrt(spread_sum / (channels * tp_count) + norm_eps)
    stats = jnp.concatenate([shifts, rstd[None]], axis=0).T
    gains = jnp.stack([v[:channels] for v in vectors])
    biases = jnp.stack([v[channels : 2 * channels] for v in vectors])
    norm_gains = jnp.stack([v[2 * channels :] for v in vectors])
    residual = project(me, conv_parts, gains, biases, stats, proj_weight, resid)

    onehot = (route_ids.reshape(-1)[:, None] == jnp.arange(sp_count, dtype=jnp.int32)[None, :]).astype(jnp.int32)
    before = jnp.cumsum(onehot, axis=0) - onehot
    position = jnp.sum(before * onehot, axis=1).reshape(tok_rows, topk_count)
    slots = (route_ids ^ sp_me) * capacity + position
    places = jnp.arange(sp_count * capacity, dtype=jnp.int32)[:, None]
    chosen = places == slots[:, 0][None, :]
    for j in range(1, topk_count):
        chosen = chosen | (places == slots[:, j][None, :])
    chosen = chosen.astype(BF16)

    group = sp_count // 4
    near = range(group)
    far = range(group, sp_count)
    away = jnp.dot(chosen[group * capacity :], residual, preferred_element_type=F32).astype(BF16)
    sent = {k: away[(k - group) * capacity : (k - group + 1) * capacity] for k in far}
    arrived = swap(sent, "sp", far)
    row_parts = spread(residual, "tp")
    close = [
        jnp.dot(chosen[: group * capacity], part, preferred_element_type=F32).astype(BF16) for part in row_parts
    ]
    close = {k: jnp.stack([c[k * capacity : (k + 1) * capacity] for c in close]) for k in near}
    close = swap(close, "sp", near)
    shared_hidden = expert_in(me, row_parts, norm_gains, shared_gate, shared_up)
    returned = []
    for g in range(4):
        members = range(g * group, (g + 1) * group)
        if g == 0:
            parts = [jnp.concatenate([close[k][p] for k in members], axis=0) for p in range(tp_count)]
        else:
            parts = spread(jnp.concatenate([arrived[k] for k in members], axis=0), "tp")
        hidden = expert_in(me, parts, norm_gains, expert_gate[0], expert_up[0])
        out = expert_out(me, spread(hidden, "tp"), expert_down[0])
        back = swap({k: out[i * capacity : (i + 1) * capacity] for i, k in enumerate(members)}, "sp", members)
        returned.append(jnp.concatenate([back[k] for k in members], axis=0))
    return combine(me, spread(shared_hidden, "tp"), shared_down, residual, slots, route_wts, returned)


def solution(mesh):
    in_specs = (
        P("sp", "tp"),
        P("sp", "tp"),
        P(None, "tp"),
        P("tp"),
        P("tp"),
        P("tp"),
        P(None, "tp"),
        P("sp", "tp"),
        P("tp"),
        P("sp", None),
        P("sp", None),
        P("sp", None, "tp"),
        P("sp", None, "tp"),
        P("sp", None, "tp"),
        P(None, "tp"),
        P(None, "tp"),
        P(None, "tp"),
    )
    out_specs = P("sp", "tp")
    return jax.shard_map(shards, mesh=mesh, in_specs=in_specs, out_specs=out_specs, check_vma=False)
```

```python
import jax
import jax.numpy as jnp
from jax import lax
from jax.experimental import pallas as pl
from jax.experimental.pallas import tpu as pltpu
from jax.sharding import PartitionSpec as P

norm_eps = 1e-06
PERMUTE_LIMIT = 8
KERNEL_VMEM = 20 << 20
F32 = jnp.float32
BF16 = jnp.bfloat16


def xor_permute(block, axis, k):
    n = lax.axis_size(axis)
    return lax.ppermute(block, axis, [(i, i ^ k) for i in range(n)])


def spread(block, axis):
    n = lax.axis_size(axis)
    if n <= PERMUTE_LIMIT:
        return [block] + [xor_permute(block, axis, k) for k in range(1, n)]
    everyone = lax.all_gather(block, axis)
    me = lax.axis_index(axis)
    return [lax.dynamic_index_in_dim(everyone, me ^ k, 0, keepdims=False) for k in range(n)]


def swap(blocks, axis):
    return {k: b if k == 0 else xor_permute(b, axis, k) for k, b in blocks.items()}


def silu(v):
    return v / (1.0 + jnp.exp(-v))


def dot(a, b):
    return jnp.dot(a, b, preferred_element_type=F32)


def member_rows(me_ref, k, width):
    return pl.ds(pl.multiple_of((me_ref[0] ^ k) * width, width), width)


class Call:
    def __init__(self, me):
        self.me, self.arrays, self.views = me, [], []

    def take(self, array):
        self.arrays.append(array)
        return len(self.arrays) - 1

    def view(self, source, pick):
        self.views.append((source, pick))
        return len(self.views) - 1

    def run(self, body, outs, scratch=()):
        count, made = len(self.arrays), len(outs)

        def kernel(me_ref, *refs):
            inputs = refs[:count]
            views = [pick(inputs[source], me_ref) for source, pick in self.views]
            body(me_ref, inputs, views, refs[count : count + made], refs[count + made :])

        return pl.pallas_call(
            kernel,
            in_specs=[pl.BlockSpec(memory_space=pltpu.SMEM)]
            + [pl.BlockSpec(memory_space=pltpu.VMEM) for _ in self.arrays],
            out_specs=[pl.BlockSpec(memory_space=pltpu.VMEM) for _ in outs],
            out_shape=list(outs),
            scratch_shapes=list(scratch),
            compiler_params=pltpu.CompilerParams(vmem_limit_bytes=KERNEL_VMEM),
        )(self.me, *self.arrays)


def convolve(me, u_val, u_gate, rim, conv_weight, conv_bias, vectors):
    rows, channels = u_val.shape
    pad, taps = rim.shape[0], conv_weight.shape[0]
    width = min(channels, rows)
    held = sum(v.shape[1] for v in vectors) // width
    call = Call(me)
    for a in (u_val, u_gate, rim, conv_weight, conv_bias.reshape(1, -1), *vectors):
        call.take(a)

    def body(me_ref, inputs, views, outs, extra):
        val_ref, gate_ref, rim_ref, weight_ref, bias_ref = inputs[:5]
        padded, sums = extra
        padded[0:pad, :] = rim_ref[...].astype(F32)
        gate = gate_ref[...].astype(F32)
        padded[pad:, :] = (val_ref[...].astype(F32) / (1.0 + jnp.exp(-gate))).astype(BF16).astype(F32)
        lanes, chunk = min(channels, 128), min(rows, 64)
        for c in range(0, channels, lanes):
            for r in range(0, rows, chunk):
                total = jnp.broadcast_to(bias_ref[:, c : c + lanes], (chunk, lanes))
                for j in range(taps):
                    at = r + pad - (taps - 1) + j
                    total = total + weight_ref[j : j + 1, c : c + lanes] * padded[at : at + chunk, c : c + lanes]
                sums[r : r + chunk, c : c + lanes] = total
        total = sums[...]
        mean = jnp.sum(total, axis=1, keepdims=True) / channels
        centred = total - mean
        squares = jnp.sum(centred * centred, axis=1, keepdims=True)
        outs[0][...] = centred.astype(BF16)
        lane = lax.broadcasted_iota(jnp.int32, (rows, 128), 1)
        stats = jnp.where(lane == 0, mean, jnp.where(lane == 1, squares, 0.0))
        outs[1][0:8, :] = stats.T[0:8, :]
        row = 8
        for ref in inputs[5:]:
            for i in range(0, ref.shape[1], width):
                outs[1][row : row + 1, 0:width] = ref[:, i : i + width]
                row += 1

    return call.run(
        body,
        [jax.ShapeDtypeStruct(u_val.shape, BF16), jax.ShapeDtypeStruct((8 + -(-held // 8) * 8, rows), F32)],
        [pltpu.VMEM((pad + rows, channels), F32), pltpu.VMEM((rows, channels), F32)],
    )


def project(me, parts, notes, proj_weight, resid, slots, group, capacity):
    n, (rows, channels), features = len(parts), parts[0].shape, resid.shape[1]
    away = range(group, lax.axis_size("sp"))
    width = min(channels, rows)
    call = Call(me)
    for a in (*parts, *notes, resid, slots):
        call.take(a)
    weight = call.take(proj_weight)
    weights = [call.view(weight, lambda ref, me_ref, k=k: ref.at[member_rows(me_ref, k, channels)]) for k in range(n)]

    def body(me_ref, inputs, views, outs, extra):
        part_refs, note_refs = inputs[:n], inputs[n : 2 * n]
        resid_ref, slot_ref = inputs[2 * n], inputs[2 * n + 1]
        means = [ref[0:1, :] for ref in note_refs]
        mean = sum(means) / n
        shifts = [m - mean for m in means]
        total = sum(ref[1:2, :] for ref in note_refs) + channels * sum(s * s for s in shifts)
        rstd = lax.rsqrt(total / (channels * n) + norm_eps)
        per = channels // width
        columns = []
        for first in range(0, n, 4):
            some = [*shifts[first : first + 4], rstd]
            some += [jnp.zeros_like(rstd)] * (8 - len(some))
            columns.append(jnp.concatenate(some, axis=0).T)
        scale = columns[0][:, min(n, 4) : min(n, 4) + 1]
        total = resid_ref[...].astype(F32)
        for k in range(n):
            shift = columns[k // 4][:, k % 4 : k % 4 + 1]
            pieces = []
            for i in range(per):
                gain = note_refs[k][8 + i : 9 + i, 0:width]
                bias = note_refs[k][8 + per + i : 9 + per + i, 0:width]
                v = (part_refs[k][:, i * width : (i + 1) * width].astype(F32) + shift) * scale
                pieces.append(silu(v * gain + bias).astype(BF16))
            weight_ref = views[weights[k]][...]
            for i in range(per):
                total = total + dot(pieces[i], weight_ref[i * width : (i + 1) * width, :])
        residual = total.astype(BF16)
        outs[0][...] = residual
        for k in range(n):
            for i in range(features // width):
                outs[1][k : k + 1, i * width : (i + 1) * width] = note_refs[k][8 + 2 * per + i : 9 + 2 * per + i, 0:width]
        places = lax.broadcasted_iota(jnp.int32, (capacity * len(away), rows), 0) + group * capacity
        chosen = places == slot_ref[0:1, :]
        for j in range(1, slot_ref.shape[0]):
            chosen = chosen | (places == slot_ref[j : j + 1, :])
        picked = dot(jnp.where(chosen, 1.0, 0.0).astype(BF16), residual).astype(BF16)
        for i in range(len(away)):
            outs[2 + i][...] = picked[i * capacity : (i + 1) * capacity, :]

    out = call.run(
        body,
        [jax.ShapeDtypeStruct(resid.shape, BF16), jax.ShapeDtypeStruct((n, features), F32)]
        + [jax.ShapeDtypeStruct((capacity, features), BF16) for _ in away],
    )
    return out[0], out[1], dict(zip(away, out[2:], strict=True))


def near_rows(me, parts, slots, group, capacity):
    n, (rows, width) = len(parts), parts[0].shape
    call = Call(me)
    for a in (*parts, slots):
        call.take(a)

    def body(me_ref, inputs, views, outs, extra):
        slot_ref = inputs[n]
        places = lax.broadcasted_iota(jnp.int32, (capacity * group, rows), 0)
        chosen = places == slot_ref[0:1, :]
        for j in range(1, slot_ref.shape[0]):
            chosen = chosen | (places == slot_ref[j : j + 1, :])
        chosen = jnp.where(chosen, 1.0, 0.0).astype(BF16)
        for p in range(n):
            picked = dot(chosen, inputs[p][...]).astype(BF16)
            for i in range(group):
                outs[i][p] = picked[i * capacity : (i + 1) * capacity, :]

    return call.run(body, [jax.ShapeDtypeStruct((n, capacity, width), BF16) for _ in range(group)])


def experts_in(me, jobs, gains):
    n, width = gains.shape
    call = Call(me)
    call.take(gains)
    plan = []
    for blocks, gate, up in jobs:
        rows = [[] for _ in range(n)]
        count = 0
        for block in blocks:
            if isinstance(block, list):
                count += block[0].shape[0]
                for k in range(n):
                    rows[k].append(call.view(call.take(block[k]), lambda ref, me_ref: ref))
            else:
                count += block.shape[1]
                source = call.take(block)
                for k in range(n):
                    rows[k].append(call.view(source, lambda ref, me_ref, k=k: ref.at[k]))
        weights = []
        for array in (gate, up):
            source = call.take(array)
            weights.append([call.view(source, lambda ref, me_ref, k=k: ref.at[member_rows(me_ref, k, width)]) for k in range(n)])
        plan.append((rows, count, *weights))
    total = sum(p[1] for p in plan)

    def body(me_ref, inputs, views, outs, extra):
        gain_ref, normed, base = inputs[0], extra[0], 0
        for rows, count, gates, ups in plan:
            at = 0
            for b in range(len(rows[0])):
                blocks = [views[here[b]] for here in rows]
                size = blocks[0].shape[0]
                chunk = min(size, 64)
                for r in range(0, size, chunk):
                    squares = 0.0
                    for ref in blocks:
                        v = ref[r : r + chunk, :].astype(F32)
                        squares = squares + jnp.sum(v * v, axis=1, keepdims=True)
                    scale = lax.rsqrt(squares / (n * width) + norm_eps)
                    for k, ref in enumerate(blocks):
                        v = ref[r : r + chunk, :].astype(F32) * scale * gain_ref[k : k + 1, :]
                        normed[at : at + chunk, k * width : (k + 1) * width] = v.astype(BF16)
                    at += chunk
            gate_sum = up_sum = 0.0
            for k in range(n):
                v = normed[0:count, k * width : (k + 1) * width]
                gate_sum = gate_sum + dot(v, views[gates[k]][...])
                up_sum = up_sum + dot(v, views[ups[k]][...])
            outs[0][base : base + count, :] = (silu(gate_sum) * up_sum).astype(BF16)
            base += count

    return call.run(
        body, [jax.ShapeDtypeStruct((total, jobs[0][1].shape[1]), BF16)],
        [pltpu.VMEM((max(p[1] for p in plan), n * width), BF16)],
    )[0]


def expert_out(me, parts, first_row, members, capacity, down):
    n, width = len(parts), parts[0].shape[1]
    count = members * capacity
    call = Call(me)
    for a in parts:
        call.take(a)
    source = call.take(down)
    downs = [call.view(source, lambda ref, me_ref, k=k: ref.at[member_rows(me_ref, k, width)]) for k in range(n)]

    def body(me_ref, inputs, views, outs, extra):
        total = 0.0
        for k in range(n):
            total = total + dot(inputs[k][first_row : first_row + count, :], views[downs[k]][...])
        total = total.astype(BF16)
        for i in range(members):
            outs[i][...] = total[i * capacity : (i + 1) * capacity, :]

    return call.run(body, [jax.ShapeDtypeStruct((capacity, down.shape[1]), BF16) for _ in range(members)])


def combine(me, parts, down, residual, slots, weights, returned):
    n, width, rows = len(parts), parts[0].shape[1], residual.shape[0]
    call = Call(me)
    for a in (residual, slots, weights, *parts):
        call.take(a)
    source = call.take(down)
    downs = [call.view(source, lambda ref, me_ref, k=k: ref.at[member_rows(me_ref, k, width)]) for k in range(n)]
    backs = [call.take(b) for b in returned]
    capacity = returned[0].shape[0]
    together = max(1, min(len(returned), 256 // capacity))

    def body(me_ref, inputs, views, outs, extra):
        residual_ref, slot_ref, weight_ref = inputs[:3]
        total = residual_ref[...].astype(F32)
        for k in range(n):
            total = total + dot(inputs[3 + k][0:rows, :], views[downs[k]][...])
        for g in range(0, len(backs), together):
            some = [inputs[i][...] for i in backs[g : g + together]]
            some = some[0] if len(some) == 1 else jnp.concatenate(some, axis=0)
            places = lax.broadcasted_iota(jnp.int32, (rows, some.shape[0]), 1) + g * capacity
            picked = 0.0
            for j in range(slot_ref.shape[1]):
                picked = picked + jnp.where(places == slot_ref[:, j : j + 1], weight_ref[:, j : j + 1], 0.0)
            high = picked.astype(BF16)
            low = (picked - high.astype(F32)).astype(BF16)
            total = total + dot(high, some) + dot(low, some)
        outs[0][...] = total.astype(BF16)

    return call.run(body, [jax.ShapeDtypeStruct(residual.shape, BF16)])[0]


def shards(
    u_val,
    u_gate,
    conv_weight,
    conv_bias,
    ln_gain,
    ln_bias,
    proj_weight,
    resid,
    norm_gain,
    route_ids,
    route_wts,
    expert_gate,
    expert_up,
    expert_down,
    shared_gate,
    shared_up,
    shared_down,
):
    tok_rows, _ = u_val.shape
    sp_count = lax.axis_size("sp")
    sp_me = lax.axis_index("sp")
    me = lax.axis_index("tp").astype(jnp.int32).reshape(1)
    reach = -(-(conv_weight.shape[0] - 1) // 16) * 16
    topk_count = route_ids.shape[1]
    capacity = 2 * tok_rows * topk_count // sp_count
    group = sp_count // 4

    val_end, gate_end = u_val[tok_rows - reach :].astype(F32), u_gate[tok_rows - reach :].astype(F32)
    ends = (val_end * jax.nn.sigmoid(gate_end)).astype(BF16)
    rim = lax.ppermute(ends, "sp", [(i, i + 1) for i in range(sp_count - 1)])
    vectors = [a.reshape(1, -1) for a in (ln_gain, ln_bias, norm_gain)]
    centred, notes = convolve(me, u_val, u_gate, rim, conv_weight, conv_bias, vectors)
    route_ids, route_wts, centred = lax.optimization_barrier((route_ids, route_wts, centred))
    conv_parts = spread(centred, "tp")
    note_parts = spread(notes, "tp")

    onehot = (route_ids.reshape(-1)[:, None] == jnp.arange(sp_count, dtype=jnp.int32)[None, :]).astype(jnp.int32)
    before = jnp.cumsum(onehot, axis=0) - onehot
    position = jnp.sum(before * onehot, axis=1).reshape(tok_rows, topk_count)
    slots = (route_ids ^ sp_me) * capacity + position
    slots_across = slots.T

    residual, gains, sent = project(me, conv_parts, note_parts, proj_weight, resid, slots_across, group, capacity)
    arrived = swap(sent, "sp")
    row_parts = spread(residual, "tp")
    close = near_rows(me, row_parts, slots_across, group, capacity)
    close = swap(dict(enumerate(close)), "sp")
    first = experts_in(
        me,
        [([row_parts], shared_gate, shared_up), ([close[k] for k in range(group)], expert_gate[0], expert_up[0])],
        gains,
    )
    first_parts = spread(first, "tp")
    returned = {}
    for g in range(4):
        members = range(g * group, (g + 1) * group)
        if g == 0:
            parts, row = first_parts, tok_rows
        else:
            rows = spread(jnp.concatenate([arrived[k] for k in members], axis=0), "tp")
            hidden = experts_in(me, [([rows], expert_gate[0], expert_up[0])], gains)
            parts, row = spread(hidden, "tp"), 0
        out = expert_out(me, parts, row, group, capacity, expert_down[0])
        returned.update(swap(dict(zip(members, out, strict=True)), "sp"))
    return combine(me, first_parts, shared_down, residual, slots, route_wts, [returned[k] for k in range(sp_count)])


def solution(mesh):
    in_specs = (
        P("sp", "tp"),
        P("sp", "tp"),
        P(None, "tp"),
        P("tp"),
        P("tp"),
        P("tp"),
        P(None, "tp"),
        P("sp", "tp"),
        P("tp"),
        P("sp", None),
        P("sp", None),
        P("sp", None, "tp"),
        P("sp", None, "tp"),
        P("sp", None, "tp"),
        P(None, "tp"),
        P(None, "tp"),
        P(None, "tp"),
    )
    out_specs = P("sp", "tp")
    return jax.shard_map(shards, mesh=mesh, in_specs=in_specs, out_specs=out_specs, check_vma=False)
```

```python
import jax
import jax.numpy as jnp
from jax import lax
from jax.experimental import pallas as pl
from jax.experimental.pallas import tpu as pltpu
from jax.sharding import PartitionSpec as P

norm_eps = 1e-06
PERMUTE_LIMIT = 8
KERNEL_VMEM = 12 << 20
F32 = jnp.float32
BF16 = jnp.bfloat16


def xor_permute(block, axis, k):
    n = lax.axis_size(axis)
    return lax.ppermute(block, axis, [(i, i ^ k) for i in range(n)])


def spread(block, axis):
    n = lax.axis_size(axis)
    if n <= PERMUTE_LIMIT:
        return [block] + [xor_permute(block, axis, k) for k in range(1, n)]
    everyone = lax.all_gather(block, axis)
    me = lax.axis_index(axis)
    return [lax.dynamic_index_in_dim(everyone, me ^ k, 0, keepdims=False) for k in range(n)]


def swap(blocks, axis):
    return {k: b if k == 0 else xor_permute(b, axis, k) for k, b in blocks.items()}


def spread_rows(blocks, axis):
    if lax.axis_size(axis) != 4:
        return [spread(jnp.concatenate(list(blocks.values()), axis=0), axis)]
    found = []
    for k, block in blocks.items():
        a = xor_permute(block, axis, 1)
        b = xor_permute(block, axis, 2)
        d = xor_permute(a, axis, 2) if k % 2 == 0 else xor_permute(b, axis, 1)
        found.append([block, a, b, d])
    return found


def silu(v):
    return v / (1.0 + jnp.exp(-v))


def dot(a, b):
    return jnp.dot(a, b, preferred_element_type=F32)


def member_rows(me_ref, k, width):
    return pl.ds(pl.multiple_of((me_ref[0] ^ k) * width, width), width)


class Call:
    def __init__(self, me):
        self.me, self.arrays, self.specs, self.views, self.copies = me, [], [], [], []

    def take(self, array):
        self.arrays.append(array)
        self.specs.append(pl.BlockSpec(memory_space=pltpu.VMEM))
        return len(self.arrays) - 1

    def view(self, source, pick):
        self.views.append((source, pick))
        return len(self.views) - 1

    def far(self, array):
        self.arrays.append(pltpu.with_memory_space_constraint(array, pltpu.HBM))
        self.specs.append(pl.BlockSpec(memory_space=pl.ANY))
        return len(self.arrays) - 1

    def copy(self, source, pick, shape):
        self.copies.append((source, pick, pltpu.VMEM(shape, self.arrays[source].dtype)))
        return len(self.copies) - 1

    def run(self, body, outs, scratch=()):
        count, made, copied = len(self.arrays), len(outs), len(self.copies)

        def kernel(me_ref, *refs):
            inputs, out_refs, extra = refs[:count], refs[count : count + made], refs[count + made :]
            started = []
            for i, (source, pick, _) in enumerate(self.copies):
                started.append(pltpu.make_async_copy(pick(inputs[source], me_ref), extra[i], extra[copied].at[i]))
                started[-1].start()

            def fetch(i):
                started[i].wait()
                return extra[i]

            views = [pick(inputs[source], me_ref) for source, pick in self.views]
            body(me_ref, inputs, views, fetch, out_refs, extra[copied + 1 :])

        return pl.pallas_call(
            kernel,
            in_specs=[pl.BlockSpec(memory_space=pltpu.SMEM), *self.specs],
            out_specs=[pl.BlockSpec(memory_space=pltpu.VMEM) for _ in outs],
            out_shape=list(outs),
            scratch_shapes=[c[2] for c in self.copies] + [pltpu.SemaphoreType.DMA((max(copied, 1),)), *scratch],
            compiler_params=pltpu.CompilerParams(vmem_limit_bytes=KERNEL_VMEM),
        )(self.me, *self.arrays)


def convolve(me, u_val, u_gate, rim, conv_weight, conv_bias, vectors):
    rows, channels = u_val.shape
    pad, taps = rim.shape[0], conv_weight.shape[0]
    width = min(channels, rows)
    held = sum(v.shape[1] for v in vectors) // width
    call = Call(me)
    call.take(rim)
    given = [u_gate, u_val, conv_weight, conv_bias.reshape(1, -1), *vectors]
    given = [call.copy(call.far(a), lambda ref, me_ref: ref, a.shape) for a in given]

    def body(me_ref, inputs, views, fetch, outs, extra):
        rim_ref = inputs[0]
        gate_ref, val_ref, weight_ref, bias_ref, *vector_refs = [fetch(i) for i in given]
        padded, sums = extra
        padded[0:pad, :] = rim_ref[...].astype(F32)
        gate = gate_ref[...].astype(F32)
        padded[pad:, :] = (val_ref[...].astype(F32) / (1.0 + jnp.exp(-gate))).astype(BF16).astype(F32)
        lanes, chunk = min(channels, 128), min(rows, 64)
        for c in range(0, channels, lanes):
            for r in range(0, rows, chunk):
                total = jnp.broadcast_to(bias_ref[:, c : c + lanes], (chunk, lanes))
                for j in range(taps):
                    at = r + pad - (taps - 1) + j
                    total = total + weight_ref[j : j + 1, c : c + lanes] * padded[at : at + chunk, c : c + lanes]
                sums[r : r + chunk, c : c + lanes] = total
        total = sums[...]
        mean = jnp.sum(total, axis=1, keepdims=True) / channels
        centred = total - mean
        squares = jnp.sum(centred * centred, axis=1, keepdims=True)
        outs[0][...] = centred.astype(BF16)
        lane = lax.broadcasted_iota(jnp.int32, (rows, 128), 1)
        stats = jnp.where(lane == 0, mean, jnp.where(lane == 1, squares, 0.0))
        outs[1][0:8, :] = stats.T[0:8, :]
        row = 8
        for ref in vector_refs:
            for i in range(0, ref.shape[1], width):
                outs[1][row : row + 1, 0:width] = ref[:, i : i + width]
                row += 1

    return call.run(
        body,
        [jax.ShapeDtypeStruct(u_val.shape, BF16), jax.ShapeDtypeStruct((8 + -(-held // 8) * 8, rows), F32)],
        [pltpu.VMEM((pad + rows, channels), F32), pltpu.VMEM((rows, channels), F32)],
    )


def project(me, parts, notes, proj_weight, resid, slots, group, capacity):
    n, (rows, channels), features = len(parts), parts[0].shape, resid.shape[1]
    away = range(group, lax.axis_size("sp"))
    width = min(channels, rows)
    call = Call(me)
    for a in (*parts, *notes, resid, slots):
        call.take(a)
    weight = call.far(proj_weight)
    weights = [
        call.copy(weight, lambda ref, me_ref, k=k: ref.at[member_rows(me_ref, k, channels)], (channels, features))
        for k in range(n)
    ]

    def body(me_ref, inputs, views, fetch, outs, extra):
        part_refs, note_refs = inputs[:n], inputs[n : 2 * n]
        resid_ref, slot_ref = inputs[2 * n], inputs[2 * n + 1]
        means = [ref[0:1, :] for ref in note_refs]
        mean = sum(means) / n
        shifts = [m - mean for m in means]
        total = sum(ref[1:2, :] for ref in note_refs) + channels * sum(s * s for s in shifts)
        rstd = lax.rsqrt(total / (channels * n) + norm_eps)
        per = channels // width
        columns = []
        for first in range(0, n, 4):
            some = [*shifts[first : first + 4], rstd]
            some += [jnp.zeros_like(rstd)] * (8 - len(some))
            columns.append(jnp.concatenate(some, axis=0).T)
        scale = columns[0][:, min(n, 4) : min(n, 4) + 1]
        normed = extra[0]
        for k in range(n):
            shift = columns[k // 4][:, k % 4 : k % 4 + 1]
            for i in range(per):
                gain = note_refs[k][8 + i : 9 + i, 0:width]
                bias = note_refs[k][8 + per + i : 9 + per + i, 0:width]
                v = (part_refs[k][:, i * width : (i + 1) * width].astype(F32) + shift) * scale
                at = k * channels + i * width
                normed[:, at : at + width] = silu(v * gain + bias).astype(BF16)
        weight_refs = [fetch(i) for i in weights]
        total = resid_ref[...].astype(F32)
        for k in range(n):
            total = total + dot(normed[:, k * channels : (k + 1) * channels], weight_refs[k][...])
        residual = total.astype(BF16)
        outs[0][...] = residual
        for k in range(n):
            for i in range(features // width):
                outs[1][k : k + 1, i * width : (i + 1) * width] = note_refs[k][8 + 2 * per + i : 9 + 2 * per + i, 0:width]
        places = lax.broadcasted_iota(jnp.int32, (capacity * len(away), rows), 0) + group * capacity
        chosen = places == slot_ref[0:1, :]
        for j in range(1, slot_ref.shape[0]):
            chosen = chosen | (places == slot_ref[j : j + 1, :])
        picked = dot(jnp.where(chosen, 1.0, 0.0).astype(BF16), residual).astype(BF16)
        for i in range(len(away)):
            outs[2 + i][...] = picked[i * capacity : (i + 1) * capacity, :]

    out = call.run(
        body,
        [jax.ShapeDtypeStruct(resid.shape, BF16), jax.ShapeDtypeStruct((n, features), F32)]
        + [jax.ShapeDtypeStruct((capacity, features), BF16) for _ in away],
        [pltpu.VMEM((rows, n * channels), BF16)],
    )
    return out[0], out[1], dict(zip(away, out[2:], strict=True))


def near_rows(me, parts, slots, group, capacity):
    n, (rows, width) = len(parts), parts[0].shape
    call = Call(me)
    for a in (*parts, slots):
        call.take(a)

    def body(me_ref, inputs, views, fetch, outs, extra):
        slot_ref = inputs[n]
        places = lax.broadcasted_iota(jnp.int32, (capacity * group, rows), 0)
        chosen = places == slot_ref[0:1, :]
        for j in range(1, slot_ref.shape[0]):
            chosen = chosen | (places == slot_ref[j : j + 1, :])
        chosen = jnp.where(chosen, 1.0, 0.0).astype(BF16)
        for p in range(n):
            picked = dot(chosen, inputs[p][...]).astype(BF16)
            for i in range(group):
                outs[i][p] = picked[i * capacity : (i + 1) * capacity, :]

    return call.run(body, [jax.ShapeDtypeStruct((n, capacity, width), BF16) for _ in range(group)])


def experts_in(me, jobs, gains):
    n, width = gains.shape
    call = Call(me)
    call.take(gains)
    plan = []
    for blocks, gate, up in jobs:
        rows = [[] for _ in range(n)]
        count = 0
        for block in blocks:
            if isinstance(block, list):
                count += block[0].shape[0]
                for k in range(n):
                    rows[k].append(call.view(call.take(block[k]), lambda ref, me_ref: ref))
            else:
                count += block.shape[1]
                source = call.take(block)
                for k in range(n):
                    rows[k].append(call.view(source, lambda ref, me_ref, k=k: ref.at[k]))
        weights = []
        for array in (gate, up):
            source = call.take(array)
            weights.append([call.view(source, lambda ref, me_ref, k=k: ref.at[member_rows(me_ref, k, width)]) for k in range(n)])
        plan.append((rows, count, *weights))
    total = sum(p[1] for p in plan)

    def body(me_ref, inputs, views, fetch, outs, extra):
        gain_ref, normed, base = inputs[0], extra[0], 0
        for rows, count, gates, ups in plan:
            at = 0
            for b in range(len(rows[0])):
                blocks = [views[here[b]] for here in rows]
                size = blocks[0].shape[0]
                chunk = min(size, 64)
                for r in range(0, size, chunk):
                    squares = 0.0
                    for ref in blocks:
                        v = ref[r : r + chunk, :].astype(F32)
                        squares = squares + jnp.sum(v * v, axis=1, keepdims=True)
                    scale = lax.rsqrt(squares / (n * width) + norm_eps)
                    for k, ref in enumerate(blocks):
                        v = ref[r : r + chunk, :].astype(F32) * scale * gain_ref[k : k + 1, :]
                        normed[at : at + chunk, k * width : (k + 1) * width] = v.astype(BF16)
                    at += chunk
            gate_sum = up_sum = 0.0
            for k in range(n):
                v = normed[0:count, k * width : (k + 1) * width]
                gate_sum = gate_sum + dot(v, views[gates[k]][...])
                up_sum = up_sum + dot(v, views[ups[k]][...])
            outs[0][base : base + count, :] = (silu(gate_sum) * up_sum).astype(BF16)
            base += count

    return call.run(
        body, [jax.ShapeDtypeStruct((total, jobs[0][1].shape[1]), BF16)],
        [pltpu.VMEM((max(p[1] for p in plan), n * width), BF16)],
    )[0]


def expert_out(me, parts, first_row, members, capacity, down):
    n, width = len(parts), parts[0].shape[1]
    count = members * capacity
    call = Call(me)
    for a in parts:
        call.take(a)
    source = call.take(down)
    downs = [call.view(source, lambda ref, me_ref, k=k: ref.at[member_rows(me_ref, k, width)]) for k in range(n)]

    def body(me_ref, inputs, views, fetch, outs, extra):
        total = 0.0
        for k in range(n):
            total = total + dot(inputs[k][first_row : first_row + count, :], views[downs[k]][...])
        total = total.astype(BF16)
        for i in range(members):
            outs[i][...] = total[i * capacity : (i + 1) * capacity, :]

    return call.run(body, [jax.ShapeDtypeStruct((capacity, down.shape[1]), BF16) for _ in range(members)])


def selection(slots, weights, first, count):
    places = lax.broadcasted_iota(jnp.int32, (slots.shape[0], count), 1) + first
    picked = 0.0
    for j in range(slots.shape[1]):
        picked = picked + jnp.where(places == slots[:, j : j + 1], weights[:, j : j + 1], 0.0)
    high = picked.astype(BF16)
    return high, (picked - high.astype(F32)).astype(BF16)


def mix(me, parts, down, residual, slots, weights, returned, late):
    n, width, rows = len(parts), parts[0].shape[1], residual.shape[0]
    capacity = next(iter(returned.values())).shape[0]
    call = Call(me)
    for a in (residual, slots, weights, *parts):
        call.take(a)
    source = call.take(down)
    downs = [call.view(source, lambda ref, me_ref, k=k: ref.at[member_rows(me_ref, k, width)]) for k in range(n)]
    pairs = []
    for k in sorted(returned):
        if pairs and pairs[-1][0] + len(pairs[-1][1]) == k and len(pairs[-1][1]) * capacity < 256:
            pairs[-1][1].append(call.take(returned[k]))
        else:
            pairs.append((k, [call.take(returned[k])]))

    def body(me_ref, inputs, views, fetch, outs, extra):
        total = inputs[0][...].astype(F32)
        slot, weight = inputs[1][...], inputs[2][...]
        for k in range(n):
            total = total + dot(inputs[3 + k][0:rows, :], views[downs[k]][...])
        for k, some in pairs:
            some = [inputs[i][...] for i in some]
            some = some[0] if len(some) == 1 else jnp.concatenate(some, axis=0)
            for part in selection(slot, weight, k * capacity, some.shape[0]):
                total = total + dot(part, some)
        outs[0][...] = total
        outs[1][...], outs[2][...] = selection(slot, weight, late[0] * capacity, len(late) * capacity)

    picked = jax.ShapeDtypeStruct((rows, len(late) * capacity), BF16)
    return call.run(body, [jax.ShapeDtypeStruct(residual.shape, F32), picked, picked])


def combine(me, total, high, low, returned):
    call = Call(me)
    for a in (total, high, low, *returned):
        call.take(a)

    def body(me_ref, inputs, views, fetch, outs, extra):
        rows = [ref[...] for ref in inputs[3:]]
        rows = rows[0] if len(rows) == 1 else jnp.concatenate(rows, axis=0)
        outs[0][...] = (inputs[0][...] + dot(inputs[1][...], rows) + dot(inputs[2][...], rows)).astype(BF16)

    return call.run(body, [jax.ShapeDtypeStruct(total.shape, BF16)])[0]


def shards(
    u_val,
    u_gate,
    conv_weight,
    conv_bias,
    ln_gain,
    ln_bias,
    proj_weight,
    resid,
    norm_gain,
    route_ids,
    route_wts,
    expert_gate,
    expert_up,
    expert_down,
    shared_gate,
    shared_up,
    shared_down,
):
    tok_rows, _ = u_val.shape
    sp_count = lax.axis_size("sp")
    sp_me = lax.axis_index("sp")
    me = lax.axis_index("tp").astype(jnp.int32).reshape(1)
    reach = -(-(conv_weight.shape[0] - 1) // 16) * 16
    topk_count = route_ids.shape[1]
    capacity = 2 * tok_rows * topk_count // sp_count
    group = sp_count // 4

    val_end, gate_end = u_val[tok_rows - reach :].astype(F32), u_gate[tok_rows - reach :].astype(F32)
    ends = (val_end * jax.nn.sigmoid(gate_end)).astype(BF16)
    rim = lax.ppermute(ends, "sp", [(i, i + 1) for i in range(sp_count - 1)])
    vectors = [a.reshape(1, -1) for a in (ln_gain, ln_bias, norm_gain)]
    centred, notes = convolve(me, u_val, u_gate, rim, conv_weight, conv_bias, vectors)
    conv_parts = spread(centred, "tp")
    note_parts = spread(notes, "tp")
    route_ids, route_wts, conv_parts[1] = lax.optimization_barrier((route_ids, route_wts, conv_parts[1]))

    onehot = (route_ids.reshape(-1)[:, None] == jnp.arange(sp_count, dtype=jnp.int32)[None, :]).astype(jnp.int32)
    before = jnp.cumsum(onehot, axis=0) - onehot
    position = jnp.sum(before * onehot, axis=1).reshape(tok_rows, topk_count)
    slots = (route_ids ^ sp_me) * capacity + position
    slots_across = slots.T

    residual, gains, sent = project(me, conv_parts, note_parts, proj_weight, resid, slots_across, group, capacity)
    arrived = swap(sent, "sp")
    row_parts = spread(residual, "tp")
    close = near_rows(me, row_parts, slots_across, group, capacity)
    close = swap(dict(enumerate(close)), "sp")
    first = experts_in(
        me,
        [([row_parts], shared_gate, shared_up), ([close[k] for k in range(group)], expert_gate[0], expert_up[0])],
        gains,
    )
    first_parts = spread(first, "tp")
    returned = {}
    for g in range(4):
        members = range(g * group, (g + 1) * group)
        if g == 0:
            parts, row = first_parts, tok_rows
        else:
            rows = spread_rows({k: arrived[k] for k in members}, "tp")
            hidden = experts_in(me, [(rows, expert_gate[0], expert_up[0])], gains)
            parts, row = spread(hidden, "tp"), 0
        out = expert_out(me, parts, row, group, capacity, expert_down[0])
        returned.update(swap(dict(zip(members, out, strict=True)), "sp"))
    late = range(group, 2 * group)
    early = {k: rows for k, rows in returned.items() if k not in late}
    total, high, low = mix(me, first_parts, shared_down, residual, slots, route_wts, early, late)
    return combine(me, total, high, low, [returned[k] for k in late])


def solution(mesh):
    in_specs = (
        P("sp", "tp"),
        P("sp", "tp"),
        P(None, "tp"),
        P("tp"),
        P("tp"),
        P("tp"),
        P(None, "tp"),
        P("sp", "tp"),
        P("tp"),
        P("sp", None),
        P("sp", None),
        P("sp", None, "tp"),
        P("sp", None, "tp"),
        P("sp", None, "tp"),
        P(None, "tp"),
        P(None, "tp"),
        P(None, "tp"),
    )
    out_specs = P("sp", "tp")
    return jax.shard_map(shards, mesh=mesh, in_specs=in_specs, out_specs=out_specs, check_vma=False)
```

```python
import jax
import jax.numpy as jnp
from jax import lax
from jax.experimental import pallas as pl
from jax.experimental.pallas import tpu as pltpu
from jax.sharding import PartitionSpec as P

norm_eps = 1e-06
PERMUTE_LIMIT = 8
KERNEL_VMEM = 8 << 20
F32 = jnp.float32
BF16 = jnp.bfloat16


def xor_permute(block, axis, k):
    n = lax.axis_size(axis)
    return lax.ppermute(block, axis, [(i, i ^ k) for i in range(n)])


def spread(block, axis):
    n = lax.axis_size(axis)
    if n <= PERMUTE_LIMIT:
        return [block] + [xor_permute(block, axis, k) for k in range(1, n)]
    everyone = lax.all_gather(block, axis)
    me = lax.axis_index(axis)
    return [lax.dynamic_index_in_dim(everyone, me ^ k, 0, keepdims=False) for k in range(n)]


def swap(blocks, axis):
    return {k: b if k == 0 else xor_permute(b, axis, k) for k, b in blocks.items()}


def spread_rows(blocks, axis):
    if lax.axis_size(axis) != 4:
        return [spread(jnp.concatenate(list(blocks.values()), axis=0), axis)]
    found = []
    for k, block in blocks.items():
        a = xor_permute(block, axis, 1)
        b = xor_permute(block, axis, 2)
        d = xor_permute(a, axis, 2) if k % 2 == 0 else xor_permute(b, axis, 1)
        found.append([block, a, b, d])
    return found


def silu(v):
    return v / (1.0 + jnp.exp(-v))


def dot(a, b):
    return jnp.dot(a, b, preferred_element_type=F32)


def member_rows(me_ref, k, width):
    return pl.ds(pl.multiple_of((me_ref[0] ^ k) * width, width), width)


def stacked(refs):
    return refs[0][...] if len(refs) == 1 else jnp.concatenate([ref[...] for ref in refs], axis=0)


class Call:
    def __init__(self, me):
        self.me, self.arrays, self.specs, self.views, self.copies = me, [], [], [], []

    def take(self, array):
        self.arrays.append(array)
        self.specs.append(pl.BlockSpec(memory_space=pltpu.VMEM))
        return len(self.arrays) - 1

    def view(self, source, pick):
        self.views.append((source, pick))
        return len(self.views) - 1

    def far(self, array):
        self.arrays.append(pltpu.with_memory_space_constraint(array, pltpu.HBM))
        self.specs.append(pl.BlockSpec(memory_space=pl.ANY))
        return len(self.arrays) - 1

    def copy(self, source, pick, shape):
        self.copies.append((source, pick, pltpu.VMEM(shape, self.arrays[source].dtype)))
        return len(self.copies) - 1

    def run(self, body, outs, scratch=()):
        count, made, copied = len(self.arrays), len(outs), len(self.copies)

        def kernel(me_ref, *refs):
            inputs, out_refs, extra = refs[:count], refs[count : count + made], refs[count + made :]
            started = []
            for i, (source, pick, _) in enumerate(self.copies):
                started.append(pltpu.make_async_copy(pick(inputs[source], me_ref), extra[i], extra[copied].at[i]))
                started[-1].start()

            def fetch(i):
                started[i].wait()
                return extra[i]

            views = [pick(inputs[source], me_ref) for source, pick in self.views]
            body(me_ref, inputs, views, fetch, out_refs, extra[copied + 1 :])

        return pl.pallas_call(
            kernel,
            in_specs=[pl.BlockSpec(memory_space=pltpu.SMEM), *self.specs],
            out_specs=[pl.BlockSpec(memory_space=pltpu.VMEM) for _ in outs],
            out_shape=list(outs),
            scratch_shapes=[c[2] for c in self.copies] + [pltpu.SemaphoreType.DMA((max(copied, 1),)), *scratch],
            compiler_params=pltpu.CompilerParams(vmem_limit_bytes=KERNEL_VMEM),
        )(self.me, *self.arrays)


def convolve(me, u_val, u_gate, rim, conv_weight, conv_bias, vectors):
    rows, channels = u_val.shape
    pad, taps = rim.shape[0], conv_weight.shape[0]
    width = min(channels, rows)
    held = sum(v.shape[1] for v in vectors) // width
    call = Call(me)
    call.take(rim)
    given = [u_gate, u_val, conv_weight, conv_bias.reshape(1, -1), *vectors]
    given = [call.copy(call.far(a), lambda ref, me_ref: ref, a.shape) for a in given]

    def body(me_ref, inputs, views, fetch, outs, extra):
        rim_ref = inputs[0]
        gate_ref, val_ref, weight_ref, bias_ref, *vector_refs = [fetch(i) for i in given]
        padded, sums = extra
        padded[0:pad, :] = rim_ref[...].astype(F32)
        gate = gate_ref[...].astype(F32)
        padded[pad:, :] = (val_ref[...].astype(F32) / (1.0 + jnp.exp(-gate))).astype(BF16).astype(F32)
        lanes, chunk = min(channels, 128), min(rows, 64)
        for c in range(0, channels, lanes):
            for r in range(0, rows, chunk):
                total = jnp.broadcast_to(bias_ref[:, c : c + lanes], (chunk, lanes))
                for j in range(taps):
                    at = r + pad - (taps - 1) + j
                    total = total + weight_ref[j : j + 1, c : c + lanes] * padded[at : at + chunk, c : c + lanes]
                sums[r : r + chunk, c : c + lanes] = total
        total = sums[...]
        mean = jnp.sum(total, axis=1, keepdims=True) / channels
        centred = total - mean
        squares = jnp.sum(centred * centred, axis=1, keepdims=True)
        outs[0][...] = centred.astype(BF16)
        lane = lax.broadcasted_iota(jnp.int32, (rows, 128), 1)
        stats = jnp.where(lane == 0, mean, jnp.where(lane == 1, squares, 0.0))
        outs[1][0:8, :] = stats.T[0:8, :]
        row = 8
        for ref in vector_refs:
            for i in range(0, ref.shape[1], width):
                outs[1][row : row + 1, 0:width] = ref[:, i : i + width]
                row += 1

    return call.run(
        body,
        [jax.ShapeDtypeStruct(u_val.shape, BF16), jax.ShapeDtypeStruct((8 + -(-held // 8) * 8, rows), F32)],
        [pltpu.VMEM((pad + rows, channels), F32), pltpu.VMEM((rows, channels), F32)],
    )


def route(me, route_ids, route_wts, experts, capacity, proj_weight):
    rows, topk = route_ids.shape
    call = Call(me)
    call.take(route_ids.T)
    call.take(route_wts.T)
    call.take(proj_weight)

    def body(me_ref, inputs, views, fetch, outs, extra):
        ids = [inputs[0][j : j + 1, :] for j in range(topk)]
        expert = lax.broadcasted_iota(jnp.int32, (experts, rows), 0)
        named = sum(jnp.where(expert == i, 1.0, 0.0) for i in ids).astype(BF16)
        earlier = lax.broadcasted_iota(jnp.int32, (rows, rows), 0) < lax.broadcasted_iota(jnp.int32, (rows, rows), 1)
        before = dot(named, jnp.where(earlier, 1.0, 0.0).astype(BF16))
        lines = []
        for j in range(topk):
            position = jnp.sum(jnp.where(expert == ids[j], before, 0.0), axis=0, keepdims=True)
            slot = (ids[j] ^ me_ref[1]) * capacity + position.astype(jnp.int32)
            outs[0][j : j + 1, :] = slot
            lines.append(slot.astype(F32))
        lines += [inputs[1][j : j + 1, :] for j in range(topk)]
        lines += [jnp.zeros_like(lines[0])] * (8 - len(lines))
        outs[1][...] = jnp.concatenate(lines, axis=0).T

    return call.run(body, [jax.ShapeDtypeStruct((topk, rows), jnp.int32), jax.ShapeDtypeStruct((rows, 8), F32)])


def project(me, parts, notes, proj_weight, resid, slots, group, capacity):
    n, (rows, channels), features = len(parts), parts[0].shape, resid.shape[1]
    away = range(group, lax.axis_size("sp"))
    width = min(channels, rows)
    call = Call(me)
    for a in (*parts, *notes, resid, slots):
        call.take(a)
    weight = call.take(proj_weight)
    weights = [call.view(weight, lambda ref, me_ref, k=k: ref.at[member_rows(me_ref, k, channels)]) for k in range(n)]

    def body(me_ref, inputs, views, fetch, outs, extra):
        part_refs, note_refs = inputs[:n], inputs[n : 2 * n]
        resid_ref, slot_ref = inputs[2 * n], inputs[2 * n + 1]
        means = [ref[0:1, :] for ref in note_refs]
        mean = sum(means) / n
        shifts = [m - mean for m in means]
        total = sum(ref[1:2, :] for ref in note_refs) + channels * sum(s * s for s in shifts)
        rstd = lax.rsqrt(total / (channels * n) + norm_eps)
        per = channels // width
        columns = []
        for first in range(0, n, 4):
            some = [*shifts[first : first + 4], rstd]
            some += [jnp.zeros_like(rstd)] * (8 - len(some))
            columns.append(jnp.concatenate(some, axis=0).T)
        scale = columns[0][:, min(n, 4) : min(n, 4) + 1]
        normed = extra[0]
        for k in range(n):
            shift = columns[k // 4][:, k % 4 : k % 4 + 1]
            for i in range(per):
                gain = note_refs[k][8 + i : 9 + i, 0:width]
                bias = note_refs[k][8 + per + i : 9 + per + i, 0:width]
                v = (part_refs[k][:, i * width : (i + 1) * width].astype(F32) + shift) * scale
                at = k * channels + i * width
                normed[:, at : at + width] = silu(v * gain + bias).astype(BF16)
        total = resid_ref[...].astype(F32)
        for k in range(n):
            total = total + dot(normed[:, k * channels : (k + 1) * channels], views[weights[k]][...])
        residual = total.astype(BF16)
        outs[0][...] = residual[0 : rows // 2, :]
        outs[1][...] = residual[rows // 2 :, :]
        for k in range(n):
            for i in range(features // width):
                outs[2][k : k + 1, i * width : (i + 1) * width] = note_refs[k][8 + 2 * per + i : 9 + 2 * per + i, 0:width]
        places = lax.broadcasted_iota(jnp.int32, (capacity * len(away), rows), 0) + group * capacity
        chosen = places == slot_ref[0:1, :]
        for j in range(1, slot_ref.shape[0]):
            chosen = chosen | (places == slot_ref[j : j + 1, :])
        picked = dot(jnp.where(chosen, 1.0, 0.0).astype(BF16), residual).astype(BF16)
        for i in range(len(away)):
            outs[3 + i][...] = picked[i * capacity : (i + 1) * capacity, :]

    out = call.run(
        body,
        [jax.ShapeDtypeStruct((rows // 2, features), BF16) for _ in range(2)]
        + [jax.ShapeDtypeStruct((n, features), F32)]
        + [jax.ShapeDtypeStruct((capacity, features), BF16) for _ in away],
        [pltpu.VMEM((rows, n * channels), BF16)],
    )
    return out[:2], out[2], dict(zip(away, out[3:], strict=True))


def near_rows(me, blocks, slots, group, capacity):
    n, width, rows = len(blocks[0]), blocks[0][0].shape[1], slots.shape[1]
    call = Call(me)
    call.take(slots)
    parts = [[call.take(block[p]) for block in blocks] for p in range(n)]

    def body(me_ref, inputs, views, fetch, outs, extra):
        slot_ref = inputs[0]
        places = lax.broadcasted_iota(jnp.int32, (capacity * group, rows), 0)
        chosen = places == slot_ref[0:1, :]
        for j in range(1, slot_ref.shape[0]):
            chosen = chosen | (places == slot_ref[j : j + 1, :])
        chosen = jnp.where(chosen, 1.0, 0.0).astype(BF16)
        for p in range(n):
            picked = dot(chosen, stacked([inputs[i] for i in parts[p]])).astype(BF16)
            for i in range(group):
                outs[i][p] = picked[i * capacity : (i + 1) * capacity, :]

    return call.run(body, [jax.ShapeDtypeStruct((n, capacity, width), BF16) for _ in range(group)])


def experts_in(me, jobs, gains):
    n, width = gains.shape
    call = Call(me)
    call.take(gains)
    plan = []
    for blocks, gate, up in jobs:
        rows = [[] for _ in range(n)]
        count = 0
        for block in blocks:
            if isinstance(block, list):
                count += block[0].shape[0]
                for k in range(n):
                    rows[k].append(call.view(call.take(block[k]), lambda ref, me_ref: ref))
            else:
                count += block.shape[1]
                source = call.take(block)
                for k in range(n):
                    rows[k].append(call.view(source, lambda ref, me_ref, k=k: ref.at[k]))
        weights = []
        for array in (gate, up):
            source = call.take(array)
            weights.append([call.view(source, lambda ref, me_ref, k=k: ref.at[member_rows(me_ref, k, width)]) for k in range(n)])
        plan.append((rows, count, *weights))
    total = sum(p[1] for p in plan)

    def body(me_ref, inputs, views, fetch, outs, extra):
        gain_ref, normed, base = inputs[0], extra[0], 0
        for rows, count, gates, ups in plan:
            at = 0
            for b in range(len(rows[0])):
                blocks = [views[here[b]] for here in rows]
                size = blocks[0].shape[0]
                chunk = min(size, 64)
                for r in range(0, size, chunk):
                    squares = 0.0
                    for ref in blocks:
                        v = ref[r : r + chunk, :].astype(F32)
                        squares = squares + jnp.sum(v * v, axis=1, keepdims=True)
                    scale = lax.rsqrt(squares / (n * width) + norm_eps)
                    for k, ref in enumerate(blocks):
                        v = ref[r : r + chunk, :].astype(F32) * scale * gain_ref[k : k + 1, :]
                        normed[at : at + chunk, k * width : (k + 1) * width] = v.astype(BF16)
                    at += chunk
            gate_sum = up_sum = 0.0
            for k in range(n):
                v = normed[0:count, k * width : (k + 1) * width]
                gate_sum = gate_sum + dot(v, views[gates[k]][...])
                up_sum = up_sum + dot(v, views[ups[k]][...])
            outs[0][base : base + count, :] = (silu(gate_sum) * up_sum).astype(BF16)
            base += count

    return call.run(
        body, [jax.ShapeDtypeStruct((total, jobs[0][1].shape[1]), BF16)],
        [pltpu.VMEM((max(p[1] for p in plan), n * width), BF16)],
    )[0]


def expert_out(me, parts, first_row, members, capacity, down):
    n, width = len(parts), parts[0].shape[1]
    count = members * capacity
    call = Call(me)
    for a in parts:
        call.take(a)
    source = call.take(down)
    downs = [call.view(source, lambda ref, me_ref, k=k: ref.at[member_rows(me_ref, k, width)]) for k in range(n)]

    def body(me_ref, inputs, views, fetch, outs, extra):
        total = 0.0
        for k in range(n):
            total = total + dot(inputs[k][first_row : first_row + count, :], views[downs[k]][...])
        total = total.astype(BF16)
        for i in range(members):
            outs[i][...] = total[i * capacity : (i + 1) * capacity, :]

    return call.run(body, [jax.ShapeDtypeStruct((capacity, down.shape[1]), BF16) for _ in range(members)])


def selection(pairs, topk, first, count):
    places = (lax.broadcasted_iota(jnp.int32, (pairs.shape[0], count), 1) + first).astype(F32)
    picked = 0.0
    for j in range(topk):
        picked = picked + jnp.where(places == pairs[:, j : j + 1], pairs[:, topk + j : topk + j + 1], 0.0)
    high = picked.astype(BF16)
    return high, (picked - high.astype(F32)).astype(BF16)


def mix(me, parts, down, residual, pairs, topk, returned, late):
    n, width, (rows, features) = len(parts), parts[0].shape[1], (pairs.shape[0], down.shape[1])
    capacity = next(iter(returned.values())).shape[0]
    call = Call(me)
    for a in (*residual, pairs, *parts):
        call.take(a)
    source = call.take(down)
    downs = [call.view(source, lambda ref, me_ref, k=k: ref.at[member_rows(me_ref, k, width)]) for k in range(n)]
    runs = []
    for k in sorted(returned):
        if runs and runs[-1][0] + len(runs[-1][1]) == k and len(runs[-1][1]) * capacity < 256:
            runs[-1][1].append(call.take(returned[k]))
        else:
            runs.append((k, [call.take(returned[k])]))

    def body(me_ref, inputs, views, fetch, outs, extra):
        total = stacked(inputs[0:2]).astype(F32)
        held = inputs[2][...]
        for k in range(n):
            total = total + dot(inputs[3 + k][0:rows, :], views[downs[k]][...])
        for k, some in runs:
            some = stacked([inputs[i] for i in some])
            for part in selection(held, topk, k * capacity, some.shape[0]):
                total = total + dot(part, some)
        outs[0][...] = total
        outs[1][...], outs[2][...] = selection(held, topk, late[0] * capacity, len(late) * capacity)

    picked = jax.ShapeDtypeStruct((rows, len(late) * capacity), BF16)
    return call.run(body, [jax.ShapeDtypeStruct((rows, features), F32), picked, picked])


def combine(me, total, high, low, returned):
    call = Call(me)
    for a in (total, high, low, *returned):
        call.take(a)

    def body(me_ref, inputs, views, fetch, outs, extra):
        rows = stacked(inputs[3:])
        outs[0][...] = (inputs[0][...] + dot(inputs[1][...], rows) + dot(inputs[2][...], rows)).astype(BF16)

    return call.run(body, [jax.ShapeDtypeStruct(total.shape, BF16)])[0]


def shards(
    u_val,
    u_gate,
    conv_weight,
    conv_bias,
    ln_gain,
    ln_bias,
    proj_weight,
    resid,
    norm_gain,
    route_ids,
    route_wts,
    expert_gate,
    expert_up,
    expert_down,
    shared_gate,
    shared_up,
    shared_down,
):
    tok_rows, _ = u_val.shape
    sp_count = lax.axis_size("sp")
    me = jnp.stack([lax.axis_index("tp"), lax.axis_index("sp")]).astype(jnp.int32)
    reach = -(-(conv_weight.shape[0] - 1) // 16) * 16
    topk_count = route_ids.shape[1]
    capacity = 2 * tok_rows * topk_count // sp_count
    group = sp_count // 4

    val_end, gate_end = u_val[tok_rows - reach :].astype(F32), u_gate[tok_rows - reach :].astype(F32)
    ends = (val_end * jax.nn.sigmoid(gate_end)).astype(BF16)
    rim = lax.ppermute(ends, "sp", [(i, i + 1) for i in range(sp_count - 1)])
    vectors = [a.reshape(1, -1) for a in (ln_gain, ln_bias, norm_gain)]
    centred, notes = convolve(me, u_val, u_gate, rim, conv_weight, conv_bias, vectors)
    conv_parts = spread(centred, "tp")
    note_parts = spread(notes, "tp")
    slots_across, pairs = route(me, route_ids, route_wts, sp_count, capacity, proj_weight)

    residual, gains, sent = project(me, conv_parts, note_parts, proj_weight, resid, slots_across, group, capacity)
    arrived = swap(sent, "sp")
    row_parts = spread_rows(dict(enumerate(residual)), "tp")
    close = near_rows(me, row_parts, slots_across, group, capacity)
    close = swap(dict(enumerate(close)), "sp")
    first = experts_in(
        me,
        [(row_parts, shared_gate, shared_up), ([close[k] for k in range(group)], expert_gate[0], expert_up[0])],
        gains,
    )
    first_parts = spread(first, "tp")
    returned = {}
    for g in range(4):
        members = range(g * group, (g + 1) * group)
        if g == 0:
            parts, row = first_parts, tok_rows
        else:
            rows = spread_rows({k: arrived[k] for k in members}, "tp")
            hidden = experts_in(me, [(rows, expert_gate[0], expert_up[0])], gains)
            parts, row = spread(hidden, "tp"), 0
        out = expert_out(me, parts, row, group, capacity, expert_down[0])
        returned.update(swap(dict(zip(members, out, strict=True)), "sp"))
    late = range(group, 2 * group)
    early = {k: rows for k, rows in returned.items() if k not in late}
    total, high, low = mix(me, first_parts, shared_down, residual, pairs, topk_count, early, late)
    return combine(me, total, high, low, [returned[k] for k in late])


def solution(mesh):
    in_specs = (
        P("sp", "tp"),
        P("sp", "tp"),
        P(None, "tp"),
        P("tp"),
        P("tp"),
        P("tp"),
        P(None, "tp"),
        P("sp", "tp"),
        P("tp"),
        P("sp", None),
        P("sp", None),
        P("sp", None, "tp"),
        P("sp", None, "tp"),
        P("sp", None, "tp"),
        P(None, "tp"),
        P(None, "tp"),
        P(None, "tp"),
    )
    out_specs = P("sp", "tp")
    return jax.shard_map(shards, mesh=mesh, in_specs=in_specs, out_specs=out_specs, check_vma=False)
```
